32 devices in a mesh: fs: 8 (over z, y), tp: 4 (over x, core).
Axes of the slice: x: 2, y: 2, z: 4, core: 2. Of those that a mesh axis runs over, the one named last changes fastest.
Arguments:
- tokens: bfloat16 [8192, 2048], P('fs', 'tp'), may hold values from -6 to 6
- norm_gain: float32 [2048], P('fs'), may hold values from 0.1 to 1.9
- up_master: float32 [2048, 4096], P('fs', 'tp'), may hold values from -0.125 to 0.125
- down_master: float32 [4096, 2048], P('fs', 'tp'), may hold values from -0.09375 to 0.09375
Outputs:
- mixed: bfloat16 [8192, 2048], P('fs', 'tp')
- up_ready: bfloat16 [2048, 4096], P(None, 'tp')
- down_ready: bfloat16 [4096, 2048], P('tp')
The draws below stay inside these ranges and needn't reach their ends.
All inputs are finite; a program needn't handle non-finite values.
Results may differ from the reference program's by a relative error of at most 0.0095.
Values may be sent and summed in bfloat16 or wider, within the bound.
A program may use at most 128 MiB of HBM per device.

```python
import jax
import jax.numpy as jnp
from jax import lax

D = 2048
FF = 4096
TOKENS = 8192
N_TP = 4


def steps_of(key, shape, shards, least, high):
    factor_of, own = 1.0, jax.random.fold_in(key, 6)
    for axis_at, blocks in shards:
        steps = jnp.exp(jax.random.uniform(jax.random.fold_in(own, axis_at), (blocks,), jnp.float32, least / len(shards), high / len(shards)))
        factor_of = factor_of * jnp.repeat(steps, shape[axis_at] // blocks).reshape([-1 if axis == axis_at else 1 for axis in range(len(shape))])
    return factor_of


def gaussian(rng, dims, spread, bound, pieces=(), held_as=jnp.bfloat16):
    loudness = steps_of(rng, dims, pieces, -0.22, 0.18) if pieces else 1.0
    array = jax.random.normal(rng, dims, jnp.float32) * spread * loudness
    return jnp.minimum(jnp.maximum(array, -bound), bound).astype(held_as)


def setup_inputs(seed: int = 0) -> dict:
    arg_keys = jax.random.split(jax.random.key(seed), 5)
    tokens = gaussian(arg_keys[0], (TOKENS, D), 1.0, 6.0, ((0, 8), (1, 4)))
    norm_gain = jnp.clip(1.0 + 0.18 * jax.random.normal(arg_keys[1], (D,), jnp.float32), 0.1, 1.9)
    up_master = gaussian(arg_keys[2], (D, FF), D ** -0.5, 0.125, ((0, 8), (1, 4)), jnp.float32)
    down_master = gaussian(arg_keys[3], (FF, D), FF ** -0.5, 0.09375, ((0, 8), (1, 4)), jnp.float32)
    return {"tokens": tokens, "norm_gain": norm_gain, "up_master": up_master, "down_master": down_master}


def reference(tokens, norm_gain, up_master, down_master):
    up_ready = (norm_gain[:, None] * up_master).astype(jnp.bfloat16)
    down_ready = down_master.astype(jnp.bfloat16)
    values = tokens.astype(jnp.float32)
    mean_square = lax.optimization_barrier(jnp.mean(values * values, axis=-1, keepdims=True))
    normed = (values * lax.rsqrt(mean_square + 1e-06)).astype(jnp.bfloat16)
    before = jnp.dot(normed, up_ready, preferred_element_type=jnp.float32)
    hidden = jnp.square(jax.nn.relu(before)).astype(jnp.bfloat16)
    block_size = FF // N_TP
    total = jnp.zeros((tokens.shape[0], D), jnp.float32)
    for block_id in range(N_TP):
        first = block_id * block_size
        partial_value = jnp.dot(hidden[:, first:first + block_size], down_ready[first:first + block_size], preferred_element_type=jnp.float32).astype(jnp.bfloat16)
        partial_value = lax.optimization_barrier(partial_value)
        total = total + partial_value.astype(jnp.float32)
    return (total.astype(jnp.bfloat16), up_ready, down_ready)
```

```python
import functools

import jax
import jax.numpy as jnp
from jax import lax
from jax.experimental import pallas as pl
from jax.experimental.pallas import tpu as pltpu
from jax.sharding import PartitionSpec as P

UP_CUTS = 2
DOWN_CUTS = 4
COLUMNS = 256
MIB = 1024 * 1024


def kernel(
    n, n_tp,
    tokens_ref, gain_ref, upm_ref, downm_ref,
    mixed_ref, upo_ref, downo_ref,
    tok, up, down, shard, scale, hidden, kept, give, take, cross, crossed, own,
    tok_send, tok_recv, gather_send, gather_recv,
    up_send, upz_recv, upy_recv,
    down_send, downz_recv, downy_recv,
    pair_send, pair_recv, cross_send, cross_recv, local_sem,
):
    f32, bf16 = jnp.float32, jnp.bfloat16
    f, t = lax.axis_index("fs"), lax.axis_index("tp")
    lines = n // 2
    z, y = f // 2, f % 2
    t1 = t + 1 - 2 * (t % 2)
    t2 = (t + 2) % 4
    t3 = (t1 + 2) % 4
    members = n // n_tp
    starts = members // 2
    owner = f // members
    above, below = (f + 2) % n, (f + n - 2) % n
    across = f + 1 - 2 * y
    has_above, has_below = z < lines - 1, z > 0

    up_rows = upm_ref.shape[0]
    down_rows = downm_ref.shape[0]
    feats = tokens_ref.shape[1]
    ucut, dcut = up_rows // UP_CUTS, down_rows // DOWN_CUTS

    def remote(src, dst, send, recv, **to):
        return pltpu.make_async_remote_copy(
            src_ref=src, dst_ref=dst, send_sem=send, recv_sem=recv,
            device_id=to, device_id_type=pl.DeviceIdType.MESH,
        )

    load = pltpu.make_async_copy(
        tokens_ref, tok.at[:, pl.ds(pl.multiple_of(t * feats, feats), feats)], local_sem.at[0]
    )
    load.start()

    shard[...] = downm_ref[...].astype(bf16)

    def down_block(source, column):
        rows = pl.ds(pl.multiple_of(source % members * down_rows, down_rows), down_rows)
        return down.at[rows, pl.ds(pl.multiple_of(column * feats, feats), feats)]

    @pl.when(owner == t)
    def _():
        down_block(f, t)[...] = downm_ref[...].astype(bf16)

    up[pl.ds(pl.multiple_of(f * up_rows, up_rows), up_rows), :] = (
        gain_ref[...] * upm_ref[...]
    ).astype(bf16)

    barrier = pltpu.get_barrier_semaphore()
    for other in (t1, t2, t3):
        pl.semaphore_signal(
            barrier, inc=1, device_id={"tp": other}, device_id_type=pl.DeviceIdType.MESH
        )
    pl.semaphore_signal(
        barrier, inc=1, device_id={"fs": across}, device_id_type=pl.DeviceIdType.MESH
    )

    @pl.when(has_above)
    def _():
        pl.semaphore_signal(
            barrier, inc=1, device_id={"fs": above}, device_id_type=pl.DeviceIdType.MESH
        )

    @pl.when(has_below)
    def _():
        pl.semaphore_signal(
            barrier, inc=1, device_id={"fs": below}, device_id_type=pl.DeviceIdType.MESH
        )

    pl.semaphore_wait(
        barrier, 4 + has_above.astype(jnp.int32) + has_below.astype(jnp.int32)
    )

    def up_piece(line, column, u):
        row = (line * 2 + column) * up_rows + u * ucut
        return up.at[pl.ds(pl.multiple_of(row, ucut), ucut), :]

    def up_copy(way, line, u, to):
        piece = up_piece(line, y, u)
        recv = upy_recv if way == 2 else upz_recv
        return remote(piece, piece, up_send.at[way, line, u], recv.at[line, u], fs=to)

    def up_onward(line, u, start):
        def go(copy):
            copy.start() if start else copy.wait_send()

        @pl.when(has_above & (line <= z))
        def _():
            go(up_copy(0, line, u, above))

        @pl.when(has_below & (line >= z))
        def _():
            go(up_copy(1, line, u, below))

        go(up_copy(2, line, u, across))

    for u in range(UP_CUTS):
        up_onward(z, u, True)

    def gather_copy(column, to):
        return remote(
            shard, down_block(f, column), gather_send.at[0], gather_recv.at[column], tp=to
        )

    @pl.when(owner != t)
    def _():
        gather_copy(t, owner).start()

    load.wait()

    def tok_copy(way, column, to):
        piece = tok.at[:, pl.ds(pl.multiple_of(column * feats, feats), feats)]
        return remote(piece, piece, tok_send.at[way], tok_recv.at[way], tp=to)

    tok_copy(1, t, t2).start()
    tok_copy(0, t, t1).start()

    @pl.loop(1, lines)
    def _(d):
        for u in range(UP_CUTS):
            @pl.when(z - d >= 0)
            def _():
                up_copy(0, z - d, u, above).wait_recv()
                up_onward(z - d, u, True)

            @pl.when(z + d < lines)
            def _():
                up_copy(1, z + d, u, below).wait_recv()
                up_onward(z + d, u, True)

    tok_copy(1, t2, t2).wait_recv()
    tok_copy(2, t2, t1).start()

    order = (t2, t3, t1, t)

    def down_piece(column, js, side, q):
        line = t * starts + js
        row = ((line * 2 + side) % members) * down_rows + q * dcut
        return down.at[
            pl.ds(pl.multiple_of(row, dcut), dcut),
            pl.ds(pl.multiple_of(column * feats, feats), feats),
        ]

    def down_copy(way, ci, js, q, to):
        piece = down_piece(order[ci], js, y, q)
        recv = downy_recv if way == 2 else downz_recv
        return remote(
            piece, piece, down_send.at[way, ci, js, q], recv.at[ci, js, q], fs=to
        )

    def down_onward(ci, js, q, start):
        line = t * starts + js

        def go(copy):
            copy.start() if start else copy.wait_send()

        @pl.when(has_above & (line <= z))
        def _():
            go(down_copy(0, ci, js, q, above))

        @pl.when(has_below & (line >= z))
        def _():
            go(down_copy(1, ci, js, q, below))

        go(down_copy(2, ci, js, q, across))

    def relay(ci, q):
        @pl.loop(0, starts)
        def _(js):
            line = t * starts + js

            if q == 0 and ci < 3:
                @pl.when(line == z)
                def _():
                    gather_copy(order[ci], t).wait_recv()

            @pl.when(line != z)
            def _():
                down_copy(0, ci, js, q, above).wait_recv()

            down_onward(ci, js, q, True)

    def relayed(ci):
        @pl.loop(0, starts)
        def _(js):
            for q in range(DOWN_CUTS):
                piece = down_piece(order[ci], js, 1 - y, q)
                remote(
                    piece, piece, down_send.at[2, ci, js, q], downy_recv.at[ci, js, q],
                    fs=across,
                ).wait_recv()

    for q in range(DOWN_CUTS):
        relay(0, q)

    tok_copy(0, t1, t1).wait_recv()
    tok_copy(2, t3, t1).wait_recv()

    rows_all = tok.shape[0]
    step = min(rows_all, 128)

    @pl.loop(0, rows_all // step)
    def _(i):
        rows = pl.ds(pl.multiple_of(i * step, step), step)
        values = tok[rows, :].astype(f32)
        mean_square = jnp.mean(values * values, axis=-1, keepdims=True)
        scale[rows, :] = lax.rsqrt(mean_square + 1e-06)

    @pl.loop(0, lines)
    def _(line):
        for u in range(UP_CUTS):
            piece = up_piece(line, 1 - y, u)
            remote(
                piece, piece, up_send.at[2, line, u], upy_recv.at[line, u], fs=across
            ).wait_recv()

    up_out = pltpu.make_async_copy(up, upo_ref, local_sem.at[1])
    up_out.start()

    width = up.shape[1]
    tiles = width // COLUMNS
    for q in range(DOWN_CUTS):
        relay(1, q)

        @pl.loop(q * tiles // DOWN_CUTS, (q + 1) * tiles // DOWN_CUTS)
        def _(i):
            columns = pl.ds(pl.multiple_of(i * COLUMNS, COLUMNS), COLUMNS)
            before = jnp.dot(tok[...], up[:, columns], preferred_element_type=f32)
            value = jnp.maximum(before * scale[...], 0.0)
            hidden[:, columns] = (value * value).astype(bf16)

    def product(ci, out):
        @pl.loop(0, feats // COLUMNS)
        def _(i):
            first = pl.multiple_of(order[ci] * feats + i * COLUMNS, COLUMNS)
            out[:, pl.ds(pl.multiple_of(i * COLUMNS, COLUMNS), COLUMNS)] = jnp.dot(
                hidden[...], down[:, pl.ds(first, COLUMNS)], preferred_element_type=f32
            ).astype(out.dtype)

    def pair_copy(i):
        return remote(give.at[i], take.at[i], pair_send.at[i], pair_recv.at[i], tp=t1)

    cross_copy = remote(cross, crossed, cross_send.at[0], cross_recv.at[0], tp=t2)

    relay(2, 0)
    relayed(0)
    product(0, kept)
    for q in range(1, DOWN_CUTS):
        relay(2, q)
    relayed(1)
    product(1, give.at[0])
    pair_copy(0).start()
    relay(3, 0)
    pair_copy(0).wait_recv()
    @pl.loop(0, rows_all // step)
    def _(i):
        rows = pl.ds(pl.multiple_of(i * step, step), step)
        cross[rows, :] = (kept[rows, :].astype(f32) + take[0, rows, :].astype(f32)).astype(bf16)

    cross_copy.start()
    for q in range(1, DOWN_CUTS):
        relay(3, q)
    relayed(2)
    product(2, give.at[1])
    pair_copy(1).start()
    relayed(3)
    down_out = pltpu.make_async_copy(down, downo_ref, local_sem.at[2])
    down_out.start()
    product(3, own)
    pair_copy(1).wait_recv()
    cross_copy.wait_recv()

    @pl.loop(0, rows_all // step)
    def _(i):
        rows = pl.ds(pl.multiple_of(i * step, step), step)
        mixed_ref[rows, :] = (
            own[rows, :] + take[1, rows, :].astype(f32) + crossed[rows, :].astype(f32)
        ).astype(bf16)

    @pl.loop(0, lines)
    def _(line):
        for u in range(UP_CUTS):
            up_onward(line, u, False)

    @pl.loop(0, starts)
    def _(js):
        for ci in range(4):
            for q in range(DOWN_CUTS):
                down_onward(ci, js, q, False)

    @pl.when(owner != t)
    def _():
        gather_copy(t, owner).wait_send()

    tok_copy(0, t, t1).wait_send()
    tok_copy(1, t, t2).wait_send()
    tok_copy(2, t2, t1).wait_send()
    pair_copy(0).wait_send()
    pair_copy(1).wait_send()
    cross_copy.wait_send()
    up_out.wait()
    down_out.wait()


def fused(n, n_tp, tokens, norm_gain, up_master, down_master):
    rows, feats = tokens.shape
    up_rows, width = up_master.shape
    down_rows = down_master.shape[0]
    depth = up_rows * n
    model = feats * n_tp
    lines, starts = n // 2, n // n_tp // 2
    bf16, f32 = jnp.bfloat16, jnp.float32
    dma = pltpu.SemaphoreType.DMA
    vmem = pl.BlockSpec(memory_space=pltpu.VMEM)
    hbm = pl.BlockSpec(memory_space=pl.ANY)
    flops = 4 * rows * depth * width
    return pl.pallas_call(
        functools.partial(kernel, n, n_tp),
        out_shape=(
            jax.ShapeDtypeStruct((rows, feats), bf16),
            jax.ShapeDtypeStruct((depth, width), bf16),
            jax.ShapeDtypeStruct((width, model), bf16),
        ),
        in_specs=[hbm, vmem, vmem, vmem],
        out_specs=(vmem, hbm, hbm),
        scratch_shapes=[
            pltpu.VMEM((rows, model), bf16),
            pltpu.VMEM((depth, width), bf16),
            pltpu.VMEM((width, model), bf16),
            pltpu.VMEM((down_rows, feats), bf16),
            pltpu.VMEM((rows, 1), f32),
            pltpu.VMEM((rows, width), bf16),
            pltpu.VMEM((rows, feats), f32),
            pltpu.VMEM((2, rows, feats), bf16),
            pltpu.VMEM((2, rows, feats), bf16),
            pltpu.VMEM((rows, feats), bf16),
            pltpu.VMEM((rows, feats), bf16),
            pltpu.VMEM((rows, feats), f32),
            dma((3,)), dma((3,)), dma((1,)), dma((n_tp,)),
            dma((3, lines, UP_CUTS)), dma((lines, UP_CUTS)), dma((lines, UP_CUTS)),
            dma((3, 4, starts, DOWN_CUTS)),
            dma((4, starts, DOWN_CUTS)), dma((4, starts, DOWN_CUTS)),
            dma((2,)), dma((2,)), dma((1,)), dma((1,)), dma((3,)),
        ],
        compiler_params=pltpu.CompilerParams(
            collective_id=0, has_side_effects=True, vmem_limit_bytes=56 * MIB
        ),
        cost_estimate=pl.CostEstimate(flops=flops, bytes_accessed=16 * MIB, transcendentals=0),
        name="layer",
    )(tokens, norm_gain[:, None], up_master, down_master)


def solution(mesh):
    n, n_tp = mesh.shape["fs"], mesh.shape["tp"]
    return jax.shard_map(
        functools.partial(fused, n, n_tp),
        mesh=mesh,
        in_specs=(P("fs", "tp"), P("fs"), P("fs", "tp"), P("fs", "tp")),
        out_specs=(P("fs", "tp"), P(None, "tp"), P("tp", None)),
        check_vma=False,
    )
```

```python
import functools

import jax
import jax.numpy as jnp
from jax import lax
from jax.experimental import pallas as pl
from jax.experimental.pallas import tpu as pltpu
from jax.sharding import PartitionSpec as P

UP_CUTS = 2
DOWN_CUTS = 2
COLUMNS = 256
LANES = 128
VMEM_LIMIT = 40
MIB = 1024 * 1024


def kernel(
    n, n_tp,
    tokens_ref, gain_ref, upm_ref, downm_ref,
    mixed_ref, up, down,
    tok, shard, scale, hidden, kept, give, take, cross, crossed, own,
    tok_send, tok_recv, gather_send, gather_recv,
    up_send, upz_recv, upy_recv,
    down_send, downz_recv, downy_recv,
    pair_send, pair_recv, cross_send, cross_recv, local_sem,
):
    f32, bf16 = jnp.float32, jnp.bfloat16
    f, t = lax.axis_index("fs"), lax.axis_index("tp")
    lines = n // 2
    z, y = f // 2, f % 2
    t1 = t + 1 - 2 * (t % 2)
    t2 = (t + 2) % 4
    t3 = (t1 + 2) % 4
    members = n // n_tp
    starts = members // 2
    owner = f // members
    above, below = (f + 2) % n, (f + n - 2) % n
    across = f + 1 - 2 * y
    has_above, has_below = z < lines - 1, z > 0

    up_rows = upm_ref.shape[0]
    down_rows = downm_ref.shape[0]
    feats = tokens_ref.shape[1]
    ucut, dcut = up_rows // UP_CUTS, down_rows // DOWN_CUTS

    def remote(src, dst, send, recv, **to):
        return pltpu.make_async_remote_copy(
            src_ref=src, dst_ref=dst, send_sem=send, recv_sem=recv,
            device_id=to, device_id_type=pl.DeviceIdType.MESH,
        )

    load = pltpu.make_async_copy(
        tokens_ref, tok.at[:, pl.ds(pl.multiple_of(t * feats, feats), feats)], local_sem.at[0]
    )
    load.start()

    shard[...] = downm_ref[...].astype(bf16)

    def down_block(source, column):
        rows = pl.ds(pl.multiple_of(source % members * down_rows, down_rows), down_rows)
        return down.at[rows, pl.ds(pl.multiple_of(column * feats, feats), feats)]

    @pl.when(owner == t)
    def _():
        down_block(f, t)[...] = downm_ref[...].astype(bf16)

    gain = jnp.transpose(jnp.broadcast_to(gain_ref[...], (LANES, up_rows)))
    for first in range(0, up.shape[1], LANES):
        up[pl.ds(pl.multiple_of(f * up_rows, up_rows), up_rows), pl.ds(first, LANES)] = (
            gain * upm_ref[:, pl.ds(first, LANES)]
        ).astype(bf16)

    barrier = pltpu.get_barrier_semaphore()
    for other in (t1, t2, t3):
        pl.semaphore_signal(
            barrier, inc=1, device_id={"tp": other}, device_id_type=pl.DeviceIdType.MESH
        )
    pl.semaphore_signal(
        barrier, inc=1, device_id={"fs": across}, device_id_type=pl.DeviceIdType.MESH
    )

    @pl.when(has_above)
    def _():
        pl.semaphore_signal(
            barrier, inc=1, device_id={"fs": above}, device_id_type=pl.DeviceIdType.MESH
        )

    @pl.when(has_below)
    def _():
        pl.semaphore_signal(
            barrier, inc=1, device_id={"fs": below}, device_id_type=pl.DeviceIdType.MESH
        )

    pl.semaphore_wait(
        barrier, 4 + has_above.astype(jnp.int32) + has_below.astype(jnp.int32)
    )

    def up_piece(line, column, u):
        row = (line * 2 + column) * up_rows + u * ucut
        return up.at[pl.ds(pl.multiple_of(row, ucut), ucut), :]

    def up_copy(way, line, u, to):
        piece = up_piece(line, y, u)
        recv = upy_recv if way == 2 else upz_recv
        return remote(piece, piece, up_send.at[way, line, u], recv.at[line, u], fs=to)

    def up_onward(line, u, start):
        def go(copy):
            copy.start() if start else copy.wait_send()

        @pl.when(has_above & (line <= z))
        def _():
            go(up_copy(0, line, u, above))

        @pl.when(has_below & (line >= z))
        def _():
            go(up_copy(1, line, u, below))

        go(up_copy(2, line, u, across))

    for u in range(UP_CUTS):
        up_onward(z, u, True)

    def gather_copy(column, to):
        return remote(
            shard, down_block(f, column), gather_send.at[0], gather_recv.at[column], tp=to
        )

    @pl.when(owner != t)
    def _():
        gather_copy(t, owner).start()

    load.wait()

    def tok_copy(way, column, to):
        piece = tok.at[:, pl.ds(pl.multiple_of(column * feats, feats), feats)]
        return remote(piece, piece, tok_send.at[way], tok_recv.at[way], tp=to)

    tok_copy(1, t, t2).start()
    tok_copy(0, t, t1).start()

    @pl.loop(1, lines)
    def _(d):
        for u in range(UP_CUTS):
            @pl.when(z - d >= 0)
            def _():
                up_copy(0, z - d, u, above).wait_recv()
                up_onward(z - d, u, True)

            @pl.when(z + d < lines)
            def _():
                up_copy(1, z + d, u, below).wait_recv()
                up_onward(z + d, u, True)

    tok_copy(1, t2, t2).wait_recv()
    tok_copy(2, t2, t1).start()

    half = feats // 2
    order = ((t2, 0), (t3, 0), (t2, 1), (t3, 1), (t1, 0), (t1, 1), (t, 0), (t, 1))

    def down_piece(ci, js, side, q):
        column, part = order[ci]
        line = t * starts + js
        row = ((line * 2 + side) % members) * down_rows + q * dcut
        return down.at[
            pl.ds(pl.multiple_of(row, dcut), dcut),
            pl.ds(pl.multiple_of(column * feats + part * half, half), half),
        ]

    def down_copy(way, ci, js, q, to):
        piece = down_piece(ci, js, y, q)
        recv = downy_recv if way == 2 else downz_recv
        return remote(
            piece, piece, down_send.at[way, ci, js, q], recv.at[ci, js, q], fs=to
        )

    def down_onward(ci, js, q, start):
        line = t * starts + js

        def go(copy):
            copy.start() if start else copy.wait_send()

        @pl.when(has_above & (line <= z))
        def _():
            go(down_copy(0, ci, js, q, above))

        @pl.when(has_below & (line >= z))
        def _():
            go(down_copy(1, ci, js, q, below))

        go(down_copy(2, ci, js, q, across))

    def relay(ci, q):
        @pl.loop(0, starts)
        def _(js):
            line = t * starts + js

            if q == 0 and ci in (0, 1, 4):
                @pl.when(line == z)
                def _():
                    gather_copy(order[ci][0], t).wait_recv()

            @pl.when(line != z)
            def _():
                down_copy(0, ci, js, q, above).wait_recv()

            down_onward(ci, js, q, True)

    def relayed(ci):
        @pl.loop(0, starts)
        def _(js):
            for q in range(DOWN_CUTS):
                piece = down_piece(ci, js, 1 - y, q)
                remote(
                    piece, piece, down_send.at[2, ci, js, q], downy_recv.at[ci, js, q],
                    fs=across,
                ).wait_recv()

    for ci in (0, 1):
        for q in range(DOWN_CUTS):
            relay(ci, q)

    tok_copy(0, t1, t1).wait_recv()
    tok_copy(2, t3, t1).wait_recv()

    rows_all = tok.shape[0]
    step = min(rows_all, 128)

    @pl.loop(0, rows_all // step)
    def _(i):
        rows = pl.ds(pl.multiple_of(i * step, step), step)
        values = tok[rows, :].astype(f32)
        mean_square = jnp.mean(values * values, axis=-1, keepdims=True)
        scale[rows, :] = lax.rsqrt(mean_square + 1e-06)

    @pl.loop(0, lines)
    def _(line):
        for u in range(UP_CUTS):
            piece = up_piece(line, 1 - y, u)
            remote(
                piece, piece, up_send.at[2, line, u], upy_recv.at[line, u], fs=across
            ).wait_recv()

    width = up.shape[1]
    tiles = width // COLUMNS
    for q in range(DOWN_CUTS):
        relay(2, q)

        @pl.loop(q * tiles // DOWN_CUTS, (q + 1) * tiles // DOWN_CUTS)
        def _(i):
            columns = pl.ds(pl.multiple_of(i * COLUMNS, COLUMNS), COLUMNS)
            before = jnp.dot(tok[...], up[:, columns], preferred_element_type=f32)
            value = jnp.maximum(before * scale[...], 0.0)
            hidden[:, columns] = (value * value).astype(bf16)

    def product(ci):
        column, part = order[ci]
        first = pl.multiple_of(column * feats + part * half, half)
        return jnp.dot(hidden[...], down[:, pl.ds(first, half)], preferred_element_type=f32)

    def pair_copy(i):
        return remote(give.at[i], take.at[i], pair_send.at[i], pair_recv.at[i], tp=t1)

    def cross_copy(i):
        return remote(
            cross.at[i], crossed.at[i], cross_send.at[i], cross_recv.at[i], tp=t2
        )

    def cross_over(i):
        pair_copy(i).wait_recv()

        @pl.loop(0, rows_all // step)
        def _(j):
            rows = pl.ds(pl.multiple_of(j * step, step), step)
            cross[i, rows, :] = (kept[rows, :] + take[i, rows, :].astype(f32)).astype(bf16)

        cross_copy(i).start()

    relay(3, 0)
    relayed(0)
    kept[...] = product(0)
    for q in range(1, DOWN_CUTS):
        relay(3, q)
    relayed(1)
    give[0] = product(1).astype(bf16)
    pair_copy(0).start()
    relay(4, 0)
    cross_over(0)
    for q in range(1, DOWN_CUTS):
        relay(4, q)
    relayed(2)
    kept[...] = product(2)
    for q in range(DOWN_CUTS):
        relay(5, q)
    relayed(3)
    give[1] = product(3).astype(bf16)
    pair_copy(1).start()
    relay(6, 0)
    cross_over(1)
    for q in range(1, DOWN_CUTS):
        relay(6, q)
    for q in range(DOWN_CUTS):
        relay(7, q)
    for ci, i in ((4, 2), (5, 3)):
        relayed(ci)
        give[i] = product(ci).astype(bf16)
        pair_copy(i).start()
    for i in range(2):
        relayed(6 + i)
        own[...] = product(6 + i)
        pair_copy(2 + i).wait_recv()
        cross_copy(i).wait_recv()

        @pl.loop(0, rows_all // step)
        def _(j):
            rows = pl.ds(pl.multiple_of(j * step, step), step)
            mixed_ref[rows, pl.ds(i * half, half)] = (
                own[rows, :] + take[2 + i, rows, :].astype(f32)
                + crossed[i, rows, :].astype(f32)
            ).astype(bf16)

    @pl.loop(0, lines)
    def _(line):
        for u in range(UP_CUTS):
            up_onward(line, u, False)

    @pl.loop(0, starts)
    def _(js):
        for ci in range(len(order)):
            for q in range(DOWN_CUTS):
                down_onward(ci, js, q, False)

    @pl.when(owner != t)
    def _():
        gather_copy(t, owner).wait_send()

    tok_copy(0, t, t1).wait_send()
    tok_copy(1, t, t2).wait_send()
    tok_copy(2, t2, t1).wait_send()
    for i in range(4):
        pair_copy(i).wait_send()
    for i in range(2):
        cross_copy(i).wait_send()


def fused(n, n_tp, tokens, norm_gain, up_master, down_master):
    rows, feats = tokens.shape
    up_rows, width = up_master.shape
    down_rows = down_master.shape[0]
    depth = up_rows * n
    model = feats * n_tp
    half = feats // 2
    lines, starts = n // 2, n // n_tp // 2
    bf16, f32 = jnp.bfloat16, jnp.float32
    dma = pltpu.SemaphoreType.DMA
    vmem = pl.BlockSpec(memory_space=pltpu.VMEM)
    hbm = pl.BlockSpec(memory_space=pl.ANY)
    flops = 4 * rows * depth * width
    return pl.pallas_call(
        functools.partial(kernel, n, n_tp),
        out_shape=(
            pltpu.VMEM((rows, feats), bf16),
            pltpu.VMEM((depth, width), bf16),
            pltpu.VMEM((width, model), bf16),
        ),
        in_specs=[hbm, vmem, vmem, vmem],
        out_specs=(vmem, vmem, vmem),
        scratch_shapes=[
            pltpu.VMEM((rows, model), bf16),
            pltpu.VMEM((down_rows, feats), bf16),
            pltpu.VMEM((rows, 1), f32),
            pltpu.VMEM((rows, width), bf16),
            pltpu.VMEM((rows, half), f32),
            pltpu.VMEM((4, rows, half), bf16),
            pltpu.VMEM((4, rows, half), bf16),
            pltpu.VMEM((2, rows, half), bf16),
            pltpu.VMEM((2, rows, half), bf16),
            pltpu.VMEM((rows, half), f32),
            dma((3,)), dma((3,)), dma((1,)), dma((n_tp,)),
            dma((3, lines, UP_CUTS)), dma((lines, UP_CUTS)), dma((lines, UP_CUTS)),
            dma((3, 8, starts, DOWN_CUTS)),
            dma((8, starts, DOWN_CUTS)), dma((8, starts, DOWN_CUTS)),
            dma((4,)), dma((4,)), dma((2,)), dma((2,)), dma((1,)),
        ],
        compiler_params=pltpu.CompilerParams(
            collective_id=0, has_side_effects=True, vmem_limit_bytes=VMEM_LIMIT * MIB
        ),
        cost_estimate=pl.CostEstimate(flops=flops, bytes_accessed=16 * MIB, transcendentals=0),
        name="layer",
    )(tokens, norm_gain[None, :], up_master, down_master)


def solution(mesh):
    n, n_tp = mesh.shape["fs"], mesh.shape["tp"]
    return jax.shard_map(
        functools.partial(fused, n, n_tp),
        mesh=mesh,
        in_specs=(P("fs", "tp"), P("fs"), P("fs", "tp"), P("fs", "tp")),
        out_specs=(P("fs", "tp"), P(None, "tp"), P("tp", None)),
        check_vma=False,
    )
```

```python
import functools

import jax
import jax.numpy as jnp
from jax import lax
from jax.experimental import pallas as pl
from jax.experimental.pallas import tpu as pltpu
from jax.sharding import PartitionSpec as P

UP_CUTS = 2
DOWN_CUTS = 2
COLUMNS = 256
LANES = 128
VMEM_LIMIT = 40
MIB = 1024 * 1024


def kernel(
    n, n_tp,
    tokens_hbm, gain_hbm, upm_hbm, downm_hbm,
    up, down, own, take, crossed,
    gain_in, upm_in, downm_in, tok, shard, scale, hidden, kept, give, cross,
    tok_send, tok_recv, gather_send, gather_recv,
    up_send, upz_recv, upy_recv, both_send, both_recv,
    down_send, downz_recv, downy_recv,
    pair_send, pair_recv, cross_send, cross_recv, local_sem,
):
    f32, bf16 = jnp.float32, jnp.bfloat16
    f, t = lax.axis_index("fs"), lax.axis_index("tp")
    lines = n // 2
    z, y = f // 2, f % 2
    t1 = t + 1 - 2 * (t % 2)
    t2 = (t + 2) % 4
    t3 = (t1 + 2) % 4
    members = n // n_tp
    starts = members // 2
    owner = f // members
    above, below = (f + 2) % n, (f + n - 2) % n
    across = f + 1 - 2 * y
    has_above, has_below = z < lines - 1, z > 0

    up_rows = upm_in.shape[0]
    down_rows = downm_in.shape[0]
    feats = tokens_hbm.shape[1]
    dcut = down_rows // DOWN_CUTS
    first_cut = max(8, up_rows // 8)
    ucuts = (first_cut, first_cut + (up_rows - first_cut) // 16 * 8, up_rows)

    def remote(src, dst, send, recv, **to):
        return pltpu.make_async_remote_copy(
            src_ref=src, dst_ref=dst, send_sem=send, recv_sem=recv,
            device_id=to, device_id_type=pl.DeviceIdType.MESH,
        )

    def down_block(source, column):
        rows = pl.ds(pl.multiple_of(source % members * down_rows, down_rows), down_rows)
        return down.at[rows, pl.ds(pl.multiple_of(column * feats, feats), feats)]

    loads = [
        pltpu.make_async_copy(upm_hbm, upm_in, local_sem.at[0]),
        pltpu.make_async_copy(gain_hbm, gain_in, local_sem.at[1]),
        pltpu.make_async_copy(downm_hbm, downm_in, local_sem.at[2]),
        pltpu.make_async_copy(
            tokens_hbm, tok.at[:, pl.ds(pl.multiple_of(t * feats, feats), feats)],
            local_sem.at[3],
        ),
    ]
    for load in loads:
        load.start()

    barrier = pltpu.get_barrier_semaphore()
    for other in (t1, t2, t3):
        pl.semaphore_signal(
            barrier, inc=1, device_id={"tp": other}, device_id_type=pl.DeviceIdType.MESH
        )
    pl.semaphore_signal(
        barrier, inc=1, device_id={"fs": across}, device_id_type=pl.DeviceIdType.MESH
    )

    @pl.when(has_above)
    def _():
        pl.semaphore_signal(
            barrier, inc=1, device_id={"fs": above}, device_id_type=pl.DeviceIdType.MESH
        )

    @pl.when(has_below)
    def _():
        pl.semaphore_signal(
            barrier, inc=1, device_id={"fs": below}, device_id_type=pl.DeviceIdType.MESH
        )

    loads[0].wait()
    loads[1].wait()
    gain = jnp.transpose(jnp.broadcast_to(gain_in[...], (LANES, up_rows)))
    for first in range(0, up.shape[1], LANES):
        up[pl.ds(pl.multiple_of(f * up_rows, up_rows), up_rows), pl.ds(first, LANES)] = (
            gain * upm_in[:, pl.ds(first, LANES)]
        ).astype(bf16)

    loads[2].wait()
    shard[...] = downm_in[...].astype(bf16)

    @pl.when(owner == t)
    def _():
        down_block(f, t)[...] = downm_in[...].astype(bf16)

    pl.semaphore_wait(
        barrier, 4 + has_above.astype(jnp.int32) + has_below.astype(jnp.int32)
    )

    def up_piece(line, column, u):
        first, last = (ucuts[u], ucuts[u + 1]) if u >= 0 else (0, ucuts[0])
        row = (line * 2 + column) * up_rows + first
        return up.at[pl.ds(pl.multiple_of(row, 8), last - first), :]

    def both_copy(way, line, column, to):
        piece = up_piece(line, column, -1)
        return remote(
            piece, piece, both_send.at[way, line, column], both_recv.at[line, column], fs=to
        )

    def both_onward(line, column, start):
        def go(copy):
            copy.start() if start else copy.wait_send()

        @pl.when(has_above & (line <= z))
        def _():
            go(both_copy(0, line, column, above))

        @pl.when(has_below & (line >= z))
        def _():
            go(both_copy(1, line, column, below))

    def up_copy(way, line, u, to):
        piece = up_piece(line, y, u)
        recv = upy_recv if way == 2 else upz_recv
        return remote(piece, piece, up_send.at[way, line, u], recv.at[line, u], fs=to)

    def up_onward(line, u, start):
        def go(copy):
            copy.start() if start else copy.wait_send()

        @pl.when(has_above & (line <= z))
        def _():
            go(up_copy(0, line, u, above))

        @pl.when(has_below & (line >= z))
        def _():
            go(up_copy(1, line, u, below))

        go(up_copy(2, line, u, across))

    both_copy(2, z, y, across).start()
    both_onward(z, y, True)
    for u in range(UP_CUTS):
        up_onward(z, u, True)

    def gather_copy(column, to):
        return remote(
            shard, down_block(f, column), gather_send.at[0], gather_recv.at[column], tp=to
        )

    @pl.when(owner != t)
    def _():
        gather_copy(t, owner).start()

    loads[3].wait()

    def tok_copy(way, column, to):
        piece = tok.at[:, pl.ds(pl.multiple_of(column * feats, feats), feats)]
        return remote(piece, piece, tok_send.at[way], tok_recv.at[way], tp=to)

    tok_copy(1, t, t2).start()
    tok_copy(0, t, t1).start()

    both_copy(2, z, 1 - y, across).wait_recv()
    both_onward(z, 1 - y, True)

    def both_relay(line, column):
        @pl.when((line >= 0) & (line < lines))
        def _():
            both_copy(0, line, column, above).wait_recv()
            both_onward(line, column, True)

    @pl.loop(1, lines)
    def _(d):
        both_relay(z - d, y)
        both_relay(z + d, y)
        for u in range(UP_CUTS):
            @pl.when(z - d >= 0)
            def _():
                up_copy(0, z - d, u, above).wait_recv()
                up_onward(z - d, u, True)

            @pl.when(z + d < lines)
            def _():
                up_copy(1, z + d, u, below).wait_recv()
                up_onward(z + d, u, True)

        both_relay(z - d, 1 - y)
        both_relay(z + d, 1 - y)

    tok_copy(1, t2, t2).wait_recv()
    tok_copy(2, t2, t1).start()

    half = feats // 2
    order = ((t2, 0), (t3, 0), (t2, 1), (t3, 1), (t1, 0), (t1, 1), (t, 0), (t, 1))

    def down_piece(ci, js, side, q):
        column, part = order[ci]
        line = t * starts + js
        row = ((line * 2 + side) % members) * down_rows + q * dcut
        return down.at[
            pl.ds(pl.multiple_of(row, dcut), dcut),
            pl.ds(pl.multiple_of(column * feats + part * half, half), half),
        ]

    def down_copy(way, ci, js, q, to):
        piece = down_piece(ci, js, y, q)
        recv = downy_recv if way == 2 else downz_recv
        return remote(
            piece, piece, down_send.at[way, ci, js, q], recv.at[ci, js, q], fs=to
        )

    def down_onward(ci, js, q, start):
        line = t * starts + js

        def go(copy):
            copy.start() if start else copy.wait_send()

        @pl.when(has_above & (line <= z))
        def _():
            go(down_copy(0, ci, js, q, above))

        @pl.when(has_below & (line >= z))
        def _():
            go(down_copy(1, ci, js, q, below))

        go(down_copy(2, ci, js, q, across))

    def relay(ci, q):
        @pl.loop(0, starts)
        def _(js):
            line = t * starts + js

            if q == 0 and ci in (0, 1, 4):
                @pl.when(line == z)
                def _():
                    gather_copy(order[ci][0], t).wait_recv()

            @pl.when(line != z)
            def _():
                down_copy(0, ci, js, q, above).wait_recv()

            down_onward(ci, js, q, True)

    def relayed(ci):
        @pl.loop(0, starts)
        def _(js):
            for q in range(DOWN_CUTS):
                piece = down_piece(ci, js, 1 - y, q)
                remote(
                    piece, piece, down_send.at[2, ci, js, q], downy_recv.at[ci, js, q],
                    fs=across,
                ).wait_recv()

    for ci in (0, 1):
        for q in range(DOWN_CUTS):
            relay(ci, q)

    tok_copy(0, t1, t1).wait_recv()
    tok_copy(2, t3, t1).wait_recv()

    rows_all = tok.shape[0]
    step = min(rows_all, 128)

    @pl.loop(0, rows_all // step)
    def _(i):
        rows = pl.ds(pl.multiple_of(i * step, step), step)
        values = tok[rows, :].astype(f32)
        mean_square = jnp.mean(values * values, axis=-1, keepdims=True)
        scale[rows, :] = lax.rsqrt(mean_square + 1e-06)

    @pl.loop(0, lines)
    def _(line):
        for u in range(UP_CUTS):
            piece = up_piece(line, 1 - y, u)
            remote(
                piece, piece, up_send.at[2, line, u], upy_recv.at[line, u], fs=across
            ).wait_recv()

    width = up.shape[1]
    tiles = width // COLUMNS
    for q in range(DOWN_CUTS):
        relay(2, q)

        @pl.loop(q * tiles // DOWN_CUTS, (q + 1) * tiles // DOWN_CUTS)
        def _(i):
            columns = pl.ds(pl.multiple_of(i * COLUMNS, COLUMNS), COLUMNS)
            before = jnp.dot(tok[...], up[:, columns], preferred_element_type=f32)
            value = jnp.maximum(before * scale[...], 0.0)
            hidden[:, columns] = (value * value).astype(bf16)

    def product(ci):
        column, part = order[ci]
        first = pl.multiple_of(column * feats + part * half, half)
        return jnp.dot(hidden[...], down[:, pl.ds(first, half)], preferred_element_type=f32)

    def pair_copy(i):
        return remote(give.at[i], take.at[i], pair_send.at[i], pair_recv.at[i], tp=t1)

    def cross_copy(i):
        return remote(
            cross.at[i], crossed.at[i], cross_send.at[i], cross_recv.at[i], tp=t2
        )

    def cross_over(i):
        pair_copy(i).wait_recv()

        @pl.loop(0, rows_all // step)
        def _(j):
            rows = pl.ds(pl.multiple_of(j * step, step), step)
            cross[i, rows, :] = (kept[rows, :] + take[i, rows, :].astype(f32)).astype(bf16)

        cross_copy(i).start()

    relay(3, 0)
    relayed(0)
    kept[...] = product(0)
    for q in range(1, DOWN_CUTS):
        relay(3, q)
    relayed(1)
    give[0] = product(1).astype(bf16)
    pair_copy(0).start()
    relay(4, 0)
    cross_over(0)
    for q in range(1, DOWN_CUTS):
        relay(4, q)
    relayed(2)
    kept[...] = product(2)
    for q in range(DOWN_CUTS):
        relay(5, q)
    relayed(3)
    give[1] = product(3).astype(bf16)
    pair_copy(1).start()
    relay(6, 0)
    cross_over(1)
    for q in range(1, DOWN_CUTS):
        relay(6, q)
    for q in range(DOWN_CUTS):
        relay(7, q)
    for ci, i in ((4, 2), (5, 3)):
        relayed(ci)
        give[i] = product(ci).astype(bf16)
        pair_copy(i).start()
    for i in range(2):
        relayed(6 + i)
        own[i] = product(6 + i)
        pair_copy(2 + i).wait_recv()
        cross_copy(i).wait_recv()

    @pl.loop(0, lines)
    def _(line):
        for u in range(UP_CUTS):
            up_onward(line, u, False)
        for column in range(2):
            both_onward(line, column, False)

    both_copy(2, z, y, across).wait_send()

    @pl.loop(0, starts)
    def _(js):
        for ci in range(len(order)):
            for q in range(DOWN_CUTS):
                down_onward(ci, js, q, False)

    @pl.when(owner != t)
    def _():
        gather_copy(t, owner).wait_send()

    tok_copy(0, t, t1).wait_send()
    tok_copy(1, t, t2).wait_send()
    tok_copy(2, t2, t1).wait_send()
    for i in range(4):
        pair_copy(i).wait_send()
    for i in range(2):
        cross_copy(i).wait_send()


def finish(up, down, own, take, crossed, mixed_hbm, up_hbm, down_hbm, mixed, sems):
    copies = [
        pltpu.make_async_copy(up, up_hbm, sems.at[0]),
        pltpu.make_async_copy(down, down_hbm, sems.at[1]),
    ]
    for copy in copies:
        copy.start()
    rows_all, half = own.shape[1:]
    step = min(rows_all, 128)
    for i in range(2):
        @pl.loop(0, rows_all // step)
        def _(j):
            rows = pl.ds(pl.multiple_of(j * step, step), step)
            mixed[rows, pl.ds(i * half, half)] = (
                own[i, rows, :] + take[2 + i, rows, :].astype(jnp.float32)
                + crossed[i, rows, :].astype(jnp.float32)
            ).astype(mixed.dtype)

    copies.append(pltpu.make_async_copy(mixed, mixed_hbm, sems.at[2]))
    copies[2].start()
    for copy in copies:
        copy.wait()


def fused(n, n_tp, tokens, norm_gain, up_master, down_master):
    rows, feats = tokens.shape
    up_rows, width = up_master.shape
    down_rows = down_master.shape[0]
    depth = up_rows * n
    model = feats * n_tp
    half = feats // 2
    lines, starts = n // 2, n // n_tp // 2
    bf16, f32 = jnp.bfloat16, jnp.float32
    dma = pltpu.SemaphoreType.DMA
    vmem = pl.BlockSpec(memory_space=pltpu.VMEM)
    hbm = pl.BlockSpec(memory_space=pltpu.HBM)
    flops = 4 * rows * depth * width
    kept = pl.pallas_call(
        functools.partial(kernel, n, n_tp),
        out_shape=(
            pltpu.VMEM((depth, width), bf16),
            pltpu.VMEM((width, model), bf16),
            pltpu.VMEM((2, rows, half), f32),
            pltpu.VMEM((4, rows, half), bf16),
            pltpu.VMEM((2, rows, half), bf16),
        ),
        in_specs=[hbm] * 4,
        out_specs=(vmem,) * 5,
        scratch_shapes=[
            pltpu.VMEM((1, up_rows), f32),
            pltpu.VMEM(up_master.shape, f32),
            pltpu.VMEM(down_master.shape, f32),
            pltpu.VMEM((rows, model), bf16),
            pltpu.VMEM((down_rows, feats), bf16),
            pltpu.VMEM((rows, 1), f32),
            pltpu.VMEM((rows, width), bf16),
            pltpu.VMEM((rows, half), f32),
            pltpu.VMEM((4, rows, half), bf16),
            pltpu.VMEM((2, rows, half), bf16),
            dma((3,)), dma((3,)), dma((1,)), dma((n_tp,)),
            dma((3, lines, UP_CUTS)), dma((lines, UP_CUTS)), dma((lines, UP_CUTS)),
            dma((3, lines, 2)), dma((lines, 2)),
            dma((3, 8, starts, DOWN_CUTS)),
            dma((8, starts, DOWN_CUTS)), dma((8, starts, DOWN_CUTS)),
            dma((4,)), dma((4,)), dma((2,)), dma((2,)), dma((4,)),
        ],
        compiler_params=pltpu.CompilerParams(
            collective_id=0, has_side_effects=True, vmem_limit_bytes=VMEM_LIMIT * MIB
        ),
        cost_estimate=pl.CostEstimate(flops=flops, bytes_accessed=16 * MIB, transcendentals=0),
        name="layer",
    )(tokens, norm_gain[None, :], up_master, down_master)
    return pl.pallas_call(
        finish,
        out_shape=(
            jax.ShapeDtypeStruct((rows, feats), bf16),
            jax.ShapeDtypeStruct((depth, width), bf16),
            jax.ShapeDtypeStruct((width, model), bf16),
        ),
        in_specs=[vmem] * 5,
        out_specs=(hbm,) * 3,
        scratch_shapes=[pltpu.VMEM((rows, feats), bf16), dma((3,))],
        compiler_params=pltpu.CompilerParams(vmem_limit_bytes=8 * MIB),
        name="finish",
    )(*kept)


def solution(mesh):
    n, n_tp = mesh.shape["fs"], mesh.shape["tp"]
    return jax.shard_map(
        functools.partial(fused, n, n_tp),
        mesh=mesh,
        in_specs=(P("fs", "tp"), P("fs"), P("fs", "tp"), P("fs", "tp")),
        out_specs=(P("fs", "tp"), P(None, "tp"), P("tp", None)),
        check_vma=False,
    )
```
